32 devices in a mesh: sp: 16 (over z, y, x), tp: 2 (over core).
Axes of the slice: x: 2, y: 2, z: 4, core: 2. Of those that a mesh axis runs over, the one named last changes fastest.
Arguments:
- residual: bfloat16 [4096, 2048], P('sp'), may hold values from -6 to 6
- queries: bfloat16 [4096, 1024], P('sp', 'tp'), may hold values from -6 to 6
- forget_gate_logits: bfloat16 [4096, 1024], P('sp', 'tp'), may hold values from -5 to 5
- projected_values: bfloat16 [4096, 1024], P('sp', 'tp'), may hold values from -6 to 6
- output_gate_logits: bfloat16 [4096, 1024], P('sp', 'tp'), may hold values from -6 to 6
- lower_bound_margin: float32 [1024], P('tp'), may hold values from 0.00024414062 to 0.08
- extra_forget_logs: float32 [4096, 1024], P('sp', 'tp'), may hold values from -0.7 to 0
- per_head_norm_gain: float32 [128], replicated, may hold values from 0.1 to 1.9
- output_weight: bfloat16 [1024, 2048], P('tp'), may hold values from -0.1875 to 0.1875
- feedforward_norm_gain: float32 [2048], replicated, may hold values from 0.1 to 1.9
- gate_weight: bfloat16 [2048, 5632], P('sp', 'tp'), may hold values from -0.125 to 0.125
- up_weight: bfloat16 [2048, 5632], P('sp', 'tp'), may hold values from -0.125 to 0.125
- down_weight: bfloat16 [5632, 2048], P('tp', 'sp'), may hold values from -0.078125 to 0.078125
Outputs:
- layer_out: bfloat16 [4096, 2048], P('sp')
The draws below stay inside these ranges and needn't reach their ends.
All inputs are finite; a program needn't handle non-finite values.
Results may differ from the reference program's by a relative error of at most 0.015.
Values may be sent and summed in bfloat16 or wider, within the bound.
A program may use at most 128 MiB of HBM per device.

```python
import math
import jax
import jax.numpy as jnp
from jax import lax

D = 2048
FF = 5632
HEADS = 8
HD = 128
HW = 1024
BLOCK = 64
TOK_DEV = 256
SEQ = 4096
N_TP = 2


def draw_lower_bound_margin(key, part):
    order = jax.random.permutation(jax.random.fold_in(key, 1), HEADS)
    slow = order < HEADS // 2
    slow_gap = 2.0 / SEQ * jax.random.uniform(jax.random.fold_in(key, 2), (HEADS, HD), jnp.float32, 0.5, 1.5)
    fast_gap = jnp.exp(jax.random.uniform(jax.random.fold_in(key, 3), (HEADS, HD), jnp.float32, math.log(0.03), math.log(0.08)))
    gaps = jnp.where(slow[:, None], slow_gap, fast_gap)
    return gaps.reshape(HW).astype(jnp.float32)


def draw_forget_gate_logits(key, part):
    base = jnp.clip(jax.random.normal(jax.random.fold_in(key, 1), (SEQ, HW), jnp.float32), -4.0, 4.0)
    shifts = jax.random.uniform(jax.random.fold_in(key, 2), (SEQ // TOK_DEV, 1, HW), jnp.float32, -1.0, 1.0)
    shifted = base.reshape(SEQ // TOK_DEV, TOK_DEV, HW) + shifts
    return shifted.reshape(SEQ, HW).astype(jnp.bfloat16)


def draw_extra_forget_logs(key, part):
    spots = jax.random.randint(jax.random.fold_in(key, 1), (4,), 0, SEQ)
    struck = jnp.any(jnp.arange(SEQ)[:, None] == spots[None, :], axis=1)
    depth = jax.random.uniform(jax.random.fold_in(key, 2), (SEQ, HW), jnp.float32, math.log(0.5), math.log(0.8))
    return jnp.where(struck[:, None], depth, 0.0).astype(jnp.float32)


def steps_of(stream_key, shape, cuts, least, largest):
    gain, own = 1.0, jax.random.fold_in(stream_key, 6)
    for axis_at, blocks in cuts:
        draws = jnp.exp(jax.random.uniform(jax.random.fold_in(own, axis_at), (blocks,), jnp.float32, least / len(cuts), largest / len(cuts)))
        gain = gain * jnp.repeat(draws, shape[axis_at] // blocks).reshape([-1 if axis == axis_at else 1 for axis in range(len(shape))])
    return gain


def centred(stream_key, shape, scale, limit, shards=(), kind=jnp.bfloat16):
    loudness = steps_of(stream_key, shape, shards, -0.22, 0.18) if shards else 1.0
    values = jax.random.normal(stream_key, shape, jnp.float32) * scale * loudness
    return jnp.minimum(jnp.maximum(values, -limit), limit).astype(kind)


def setup_inputs(seed: int = 0) -> dict:
    arg_keys = jax.random.split(jax.random.key(seed), 14)
    return {
        "residual": centred(arg_keys[0], (SEQ, D), 1.0, 6.0, ((0, 16),)),
        "queries": centred(arg_keys[1], (SEQ, HW), 1.0, 6.0, ((0, 16), (1, 2))),
        "forget_gate_logits": draw_forget_gate_logits(jax.random.fold_in(arg_keys[13], 71), 0),
        "projected_values": centred(arg_keys[3], (SEQ, HW), 1.0, 6.0, ((0, 16), (1, 2))),
        "output_gate_logits": centred(arg_keys[4], (SEQ, HW), 1.0, 6.0, ((0, 16), (1, 2))),
        "lower_bound_margin": draw_lower_bound_margin(jax.random.fold_in(arg_keys[13], 71), 0),
        "extra_forget_logs": draw_extra_forget_logs(jax.random.fold_in(arg_keys[13], 71), 0),
        "per_head_norm_gain": jnp.clip(1.0 + 0.18 * jax.random.normal(arg_keys[7], (HD,), jnp.float32), 0.1, 1.9),
        "output_weight": centred(arg_keys[8], (HW, D), HW ** -0.5, 0.1875, ((0, 2),)),
        "feedforward_norm_gain": jnp.clip(1.0 + 0.18 * jax.random.normal(arg_keys[9], (D,), jnp.float32), 0.1, 1.9),
        "gate_weight": centred(arg_keys[10], (D, FF), D ** -0.5, 0.125, ((0, 16), (1, 2))),
        "up_weight": centred(arg_keys[11], (D, FF), D ** -0.5, 0.125, ((0, 16), (1, 2))),
        "down_weight": centred(arg_keys[12], (FF, D), FF ** -0.5, 0.078125, ((0, 2), (1, 16))),
    }


eps = 1e-06
top_precision = lax.Precision.HIGHEST

def block_update(recurrent_state, inputs):
    queries, state_increment, value_rows, retain_log_factor = inputs
    running_state = jnp.cumsum(retain_log_factor, axis=1)
    causal = jnp.tril(jnp.ones((retain_log_factor.shape[1], retain_log_factor.shape[1]), dtype=bool))
    carried_over_state = jnp.einsum('uqw,uwa->uqa', queries * jnp.exp(running_state), recurrent_state, precision=top_precision)
    spread = running_state[:, :, None, :] - running_state[:, None, :, :]
    weights = jnp.exp(jnp.where(causal[None, :, :, None], spread, -jnp.inf))
    scores = jnp.einsum('htk,htsk,hsk->hts', queries, weights, state_increment, precision=top_precision)
    output_rows = carried_over_state + jnp.einsum('hts,hsv->htv', scores, value_rows, precision=top_precision)
    final_state = running_state[:, -1:, :]
    updated_state = jnp.exp(final_state[:, 0, :])[:, :, None] * recurrent_state + jnp.einsum('erb,erc->ebc', state_increment * jnp.exp(final_state - running_state), value_rows, precision=top_precision)
    return (updated_state, output_rows)

def grouped_product(left, right, groups):
    group_width = left.shape[1] // groups
    summed = jnp.zeros((left.shape[0], right.shape[1]), jnp.float32)
    for member in range(groups):
        lower = member * group_width
        upper = lower + group_width
        part_product = jnp.dot(left[:, lower:upper], right[lower:upper], preferred_element_type=jnp.float32)
        rounded = lax.optimization_barrier(part_product.astype(jnp.bfloat16))
        summed = summed + rounded.astype(jnp.float32)
    return summed

def reference(residual, queries, forget_gate_logits, projected_values, output_gate_logits, lower_bound_margin, extra_forget_logs, per_head_norm_gain, output_weight, feedforward_norm_gain, gate_weight, up_weight, down_weight):
    state_increment = lower_bound_margin * jax.nn.sigmoid(-forget_gate_logits.astype(jnp.float32))
    retain_log_factor = jnp.log1p(-state_increment) + extra_forget_logs

    def to_blocks(source):
        return source.reshape(SEQ // BLOCK, BLOCK, HEADS, HD).transpose(0, 2, 1, 3)
    initial = jnp.zeros((HEADS, HD, HD), jnp.float32)
    block_inputs = (to_blocks(queries.astype(jnp.float32)), to_blocks(state_increment), to_blocks(projected_values.astype(jnp.float32)), to_blocks(retain_log_factor))
    _, output_rows = lax.scan(block_update, initial, block_inputs)
    mixed = output_rows.transpose(0, 2, 1, 3).reshape(SEQ, HEADS, HD)
    normed_heads = mixed * lax.rsqrt(lax.optimization_barrier(jnp.mean(mixed * mixed, axis=-1, keepdims=True)) + eps) * per_head_norm_gain
    gating = jax.nn.silu(output_gate_logits.astype(jnp.float32)).reshape(SEQ, HEADS, HD)
    gated = (normed_heads * gating).reshape(SEQ, HW).astype(jnp.bfloat16)
    projected = grouped_product(gated, output_weight, N_TP)
    after_mixer = (residual.astype(jnp.float32) + projected).astype(jnp.bfloat16)
    widened = after_mixer.astype(jnp.float32)
    normed = (widened * lax.rsqrt(lax.optimization_barrier(jnp.mean(widened * widened, axis=-1, keepdims=True)) + eps) * feedforward_norm_gain).astype(jnp.bfloat16)
    group_width = FF // N_TP
    ffn_sum = jnp.zeros((SEQ, D), jnp.float32)
    for member in range(N_TP):
        lower = member * group_width
        upper = lower + group_width
        gate_part = jnp.dot(normed, gate_weight[:, lower:upper], preferred_element_type=jnp.float32)
        up_part = jnp.dot(normed, up_weight[:, lower:upper], preferred_element_type=jnp.float32)
        hidden = (jax.nn.silu(gate_part) * up_part).astype(jnp.bfloat16)
        part_product = jnp.dot(hidden, down_weight[lower:upper], preferred_element_type=jnp.float32)
        rounded = lax.optimization_barrier(part_product.astype(jnp.bfloat16))
        ffn_sum = ffn_sum + rounded.astype(jnp.float32)
    return (after_mixer.astype(jnp.float32) + 0.5 * ffn_sum).astype(jnp.bfloat16)
```

```python
import jax
import jax.numpy as jnp
from jax import lax
from jax.experimental import pallas as pl
from jax.experimental.pallas import tpu as pltpu
from jax.sharding import PartitionSpec as P

HD = 128
BLOCK = 64


eps = 1e-06
top_precision = lax.Precision.HIGHEST


def carried_in_2(value, axis, join, neutral):
    place = lax.axis_index(axis)
    gathered = jax.tree.map(
        lambda a, kind: lax.all_gather(a.astype(kind), axis), value, (jnp.bfloat16, jnp.bfloat16)
    )
    state = jax.tree.map(lambda a, e: jnp.zeros_like(a) + jnp.asarray(e, a.dtype), value, neutral)

    def one(turn, state):
        return join(
            state,
            jax.tree.map(
                lambda a, own: lax.dynamic_index_in_dim(a, turn, 0, False).astype(own.dtype),
                gathered,
                value,
            ),
        )

    return lax.fori_loop(0, place, one, state)


def block_update(carried_in, inputs):
    recurrent_state, offset = carried_in
    queries, state_increment, value_rows, retain_log_factor = inputs
    running_state = jnp.cumsum(retain_log_factor, axis=1)
    causal = jnp.tril(
        jnp.ones((retain_log_factor.shape[1], retain_log_factor.shape[1]), dtype=bool)
    )
    carried_over_state = jnp.einsum(
        "uqw,uwa->uqa", queries * jnp.exp(running_state), recurrent_state, precision=top_precision
    )
    spread = running_state[:, :, None, :] - running_state[:, None, :, :]
    weights = jnp.exp(jnp.where(causal[None, :, :, None], spread, -jnp.inf))
    scores = jnp.einsum(
        "htk,htsk,hsk->hts", queries, weights, state_increment, precision=top_precision
    )
    output_rows = carried_over_state + jnp.einsum(
        "hts,hsv->htv", scores, value_rows, precision=top_precision
    )
    final_state = running_state[:, -1:, :]
    updated_state = jnp.exp(final_state[:, 0, :])[:, :, None] * recurrent_state + jnp.einsum(
        "erb,erc->ebc",
        state_increment * jnp.exp(final_state - running_state),
        value_rows,
        precision=top_precision,
    )
    rescaled_state = queries * jnp.exp(running_state + offset[:, None, :])
    return ((updated_state, offset + final_state[:, 0, :]), (output_rows, rescaled_state))


def join_states(earlier, later):
    earlier_sum, earlier_memory = earlier
    later_sum, later_memory = later
    return (earlier_sum + later_sum, jnp.exp(later_sum)[:, :, None] * earlier_memory + later_memory)


MESH = pl.DeviceIdType.MESH
GROUPS = 4


def up_to(value, step):
    return -(-value // step) * step


def feed_forward_kernel(
    dims, gu_ref, dn_ref, x_ref, nrm_ref, out_ref,
    gu, dn, rows_in, hid, part, peer_part, summed, got,
    s_a, r_a, s_b, r_b, s_x, r_x, s_p, r_p, s_d, r_d, s_r, r_r, s_o, r_o, s_l,
):
    n_r, share, own, width, padded = dims
    me = lax.axis_index("sp")
    c = lax.axis_index("tp")
    h, r = me // n_r, me % n_r
    model = gu.shape[0]

    def away(d):
        return (h + d) % GROUPS

    def back(d):
        return (h + GROUPS - d) % GROUPS

    def beside(e):
        return ((r // 2 + e // 2) % 2) * 2 + (r % 2 + e % 2) % 2

    def remote(src, dst, send, recv, hh, rr, cc):
        return pltpu.make_async_remote_copy(
            src_ref=src, dst_ref=dst, send_sem=send, recv_sem=recv,
            device_id=(hh * n_r + rr, cc), device_id_type=MESH,
        )

    def gu_rows(owner):
        return gu.at[pl.ds(pl.multiple_of(owner * share, share), share)]

    def dn_cols(owner):
        return dn.at[pl.ds(0, width), pl.ds(pl.multiple_of(owner * share, share), share)]

    def token_rows(hh, cc):
        return pl.ds(pl.multiple_of((hh * 2 + cc) * own, own), own)

    started = []

    def go(copy):
        copy.start()
        started.append(copy)
        return copy

    weights_a = {}
    weights_b = {}
    for d in (1, 3, 2):
        weights_a[d, 0] = go(remote(gu_ref.at[away(d)], gu_rows(me), s_a.at[d - 1, 0], r_a.at[d - 1, 0], away(d), r, c))
    acts = {}
    for d in (1, 3, 2):
        acts[d] = go(remote(nrm_ref, rows_in.at[token_rows(h, c)], s_x.at[d - 1], r_x.at[d - 1], away(d), r, c))
    peers = {0: go(remote(nrm_ref, rows_in.at[token_rows(h, c)], s_p.at[0], r_p.at[0], h, r, 1 - c))}
    for d in (1, 3, 2):
        weights_a[d, 1] = go(remote(dn_ref.at[away(d)], dn_cols(me), s_a.at[d - 1, 1], r_a.at[d - 1, 1], away(d), r, c))
    own_gu = pltpu.make_async_copy(gu_ref.at[h], gu_rows(me), s_l.at[0])
    own_dn = pltpu.make_async_copy(dn_ref.at[h], dn_cols(me), s_l.at[1])
    own_gu.start()
    own_dn.start()
    for e in (1, 2, 3):
        weights_b[0, e, 0] = go(remote(gu_ref.at[h], gu_rows(me), s_b.at[0, e - 1, 0], r_b.at[0, e - 1, 0], h, beside(e), c))
    rows_in[token_rows(h, c), :] = nrm_ref[...]
    dn[pl.ds(width, padded - width), :] = jnp.zeros((padded - width, model), dn.dtype)
    for k in range(2):
        if k == 1:
            for e in (1, 2, 3):
                weights_b[0, e, 1] = go(remote(dn_ref.at[h], dn_cols(me), s_b.at[0, e - 1, 1], r_b.at[0, e - 1, 1], h, beside(e), c))
        for d in (1, 3, 2):
            weights_a[d, k].wait_recv()
            block = (gu_rows if k == 0 else dn_cols)(back(d) * n_r + r)
            for e in (1, 2, 3):
                weights_b[d, e, k] = go(remote(block, block, s_b.at[d, e - 1, k], r_b.at[d, e - 1, k], h, beside(e), c))
        if k == 0:
            for d in (1, 3, 2):
                acts[d].wait_recv()
                block = rows_in.at[token_rows(back(d), c)]
                peers[d] = go(remote(block, block, s_p.at[d], r_p.at[d], h, r, 1 - c))
    own_gu.wait()
    own_dn.wait()
    for d in range(4):
        for e in (1, 2, 3):
            weights_b[d, e, 0].wait_recv()

    def reduce_block(d, exchange):
        exchange.wait_recv()
        here = part[d, pl.ds(pl.multiple_of(c * own, own), own), :]
        total = here.astype(jnp.float32) + peer_part[d].astype(jnp.float32)
        summed[d] = total.astype(jnp.bfloat16)
        if d == 0:
            return None
        return go(remote(summed.at[d], got.at[d - 1], s_r.at[d - 1], r_r.at[d - 1], back(d), r, c))

    tile = 256
    order = (1, 3, 2, 0)
    exchanges = {}
    reduced = {}
    for place, d in enumerate(order):
        peers[d].wait_recv()
        first = pl.multiple_of(back(d) * 2 * own, 2 * own)

        def gate_up(j, carry):
            at = pl.multiple_of(j * tile, tile)
            rows = rows_in[pl.ds(first, 2 * own), :]
            gate = jnp.dot(rows, gu[:, pl.ds(at, tile)], preferred_element_type=jnp.float32)
            up = jnp.dot(rows, gu[:, pl.ds(padded + at, tile)], preferred_element_type=jnp.float32)
            hid[:, pl.ds(at, tile)] = (gate * jax.nn.sigmoid(gate) * up).astype(jnp.bfloat16)
            return carry

        lax.fori_loop(0, padded // tile, gate_up, 0)
        if place == 0:
            for dd in range(4):
                for e in (1, 2, 3):
                    weights_b[dd, e, 1].wait_recv()

        def down(j, carry):
            at = pl.multiple_of(j * tile, tile)
            part[d, :, pl.ds(at, tile)] = jnp.dot(
                hid[...], dn[:, pl.ds(at, tile)], preferred_element_type=jnp.float32
            ).astype(jnp.bfloat16)
            return carry

        lax.fori_loop(0, model // tile, down, 0)
        exchanges[d] = go(remote(
            part.at[d, pl.ds(pl.multiple_of((1 - c) * own, own), own)], peer_part.at[d],
            s_d.at[d], r_d.at[d], h, r, 1 - c,
        ))
        if place:
            reduced[order[place - 1]] = reduce_block(order[place - 1], exchanges[order[place - 1]])
    reduce_block(0, exchanges[0])
    total = summed[0].astype(jnp.float32)
    for d in (1, 3, 2):
        reduced[d].wait_recv()
        total = total + got[d - 1].astype(jnp.float32)
    mine = pl.ds(pl.multiple_of(c * own, own), own)
    out_ref[mine, :] = (x_ref[...].astype(jnp.float32) + 0.5 * total).astype(jnp.bfloat16)
    finish = go(remote(out_ref.at[mine], out_ref.at[mine], s_o.at[0], r_o.at[0], h, r, 1 - c))
    finish.wait_recv()
    for copy in started:
        copy.wait_send()


def feed_forward(gate_weight, up_weight, down_weight, after_mixer, normed):
    n_sp = lax.axis_size("sp")
    share, half = gate_weight.shape
    width = half // GROUPS
    padded = up_to(width, 256)
    own, model = normed.shape
    pad = ((0, 0), (0, 0), (0, padded - width))
    split = lambda w: jnp.pad(w.reshape(share, GROUPS, width), pad)
    gu = jnp.concatenate([split(gate_weight), split(up_weight)], axis=2).transpose(1, 0, 2)
    dn = down_weight.reshape(GROUPS, width, share)
    bf = jnp.bfloat16
    dma = pltpu.SemaphoreType.DMA
    dims = (n_sp // GROUPS, share, own, width, padded)
    vm = pl.BlockSpec(memory_space=pltpu.VMEM)
    hbm = pl.BlockSpec(memory_space=pl.ANY)
    return pl.pallas_call(
        lambda *refs: feed_forward_kernel(dims, *refs),
        out_shape=jax.ShapeDtypeStruct((2 * own, model), bf),
        in_specs=[hbm, hbm, vm, vm],
        out_specs=vm,
        scratch_shapes=[
            pltpu.VMEM((model, 2 * padded), bf),
            pltpu.VMEM((padded, model), bf),
            pltpu.VMEM((GROUPS * 2 * own, model), bf),
            pltpu.VMEM((2 * own, padded), bf),
            pltpu.VMEM((GROUPS, 2 * own, model), bf),
            pltpu.VMEM((GROUPS, own, model), bf),
            pltpu.VMEM((GROUPS, own, model), bf),
            pltpu.VMEM((GROUPS - 1, own, model), bf),
            dma((3, 2)), dma((3, 2)), dma((4, 3, 2)), dma((4, 3, 2)),
            dma((3,)), dma((3,)), dma((4,)), dma((4,)), dma((4,)), dma((4,)),
            dma((3,)), dma((3,)), dma((1,)), dma((1,)), dma((2,)),
        ],
        compiler_params=pltpu.CompilerParams(has_side_effects=True, vmem_limit_bytes=56 * 2**20),
    )(gu, dn, after_mixer, normed)


def fits(mesh, share, own, width):
    return (
        mesh["sp"] == 4 * GROUPS and mesh["tp"] == 2
        and share % 128 == 0 and own % 16 == 0 and width % 16 == 0
    )


def local(
    residual,
    queries,
    forget_gate_logits,
    projected_values,
    output_gate_logits,
    lower_bound_margin,
    extra_forget_logs,
    per_head_norm_gain,
    output_weight,
    feedforward_norm_gain,
    gate_weight,
    up_weight,
    down_weight,
):
    length = queries.shape[0]
    head_count = queries.shape[1] // HD
    state_increment = lower_bound_margin * jax.nn.sigmoid(-forget_gate_logits.astype(jnp.float32))
    retain_log_factor = jnp.log1p(-state_increment) + extra_forget_logs

    def to_blocks(source):
        return source.reshape(length // BLOCK, BLOCK, head_count, HD).transpose(0, 2, 1, 3)

    initial = (
        jnp.zeros((head_count, HD, HD), jnp.float32),
        jnp.zeros((head_count, HD), jnp.float32),
    )
    block_inputs = (
        to_blocks(queries.astype(jnp.float32)),
        to_blocks(state_increment),
        to_blocks(projected_values.astype(jnp.float32)),
        to_blocks(retain_log_factor),
    )
    (recurrent_state, decay_sum), (output_rows, rescaled_state) = lax.scan(
        block_update, initial, block_inputs
    )
    identity = (jnp.zeros_like(decay_sum), jnp.zeros_like(recurrent_state))
    incoming_state = carried_in_2((decay_sum, recurrent_state), "sp", join_states, identity)[1]
    output_rows = output_rows + jnp.einsum(
        "sjey,jyx->sjex", rescaled_state, incoming_state, precision=top_precision
    )
    mixed = output_rows.transpose(0, 2, 1, 3).reshape(length, head_count, HD)
    normed_heads = (
        mixed
        * lax.rsqrt(jnp.mean(mixed * mixed, axis=-1, keepdims=True) + eps)
        * per_head_norm_gain
    )
    gating = jax.nn.silu(output_gate_logits.astype(jnp.float32)).reshape(length, head_count, HD)
    gated = (normed_heads * gating).reshape(length, head_count * HD).astype(jnp.bfloat16)
    row_count = residual.shape[0] // lax.axis_size("tp")
    own_rows = lax.dynamic_slice_in_dim(residual, lax.axis_index("tp") * row_count, row_count, 0)
    rows_here = gated
    projected = lax.psum_scatter(
        jnp.dot(rows_here, output_weight, preferred_element_type=jnp.float32).astype(jnp.bfloat16),
        "tp",
        scatter_dimension=0,
        tiled=True,
    ).astype(jnp.float32)
    after_mixer = (own_rows.astype(jnp.float32) + projected).astype(jnp.bfloat16)
    widened = after_mixer.astype(jnp.float32)
    normed = (
        widened
        * lax.rsqrt(jnp.mean(widened * widened, axis=-1, keepdims=True) + eps)
        * feedforward_norm_gain
    ).astype(jnp.bfloat16)
    sizes = {"sp": lax.axis_size("sp"), "tp": lax.axis_size("tp")}
    if fits(sizes, gate_weight.shape[0], row_count, gate_weight.shape[1] // GROUPS):
        return feed_forward(gate_weight, up_weight, down_weight, after_mixer, normed)
    gate_full, up_full = (
        lax.all_gather(gate_weight, "sp", axis=0, tiled=True),
        lax.all_gather(up_weight, "sp", axis=0, tiled=True),
    )
    down_full = lax.all_gather(down_weight, "sp", axis=1, tiled=True)
    row_piece = lax.all_gather(normed, "tp", axis=0, tiled=True)
    gate_part = jnp.dot(row_piece, gate_full, preferred_element_type=jnp.float32)
    up_part = jnp.dot(row_piece, up_full, preferred_element_type=jnp.float32)
    hidden = (jax.nn.silu(gate_part) * up_part).astype(jnp.bfloat16)
    rows_here = hidden
    ffn_sum = lax.psum_scatter(
        jnp.dot(rows_here, down_full, preferred_element_type=jnp.float32).astype(jnp.bfloat16),
        "tp",
        scatter_dimension=0,
        tiled=True,
    ).astype(jnp.float32)
    finished = (after_mixer.astype(jnp.float32) + 0.5 * ffn_sum).astype(jnp.bfloat16)
    return lax.all_gather(finished, "tp", axis=0, tiled=True)


def solution(mesh):
    return jax.shard_map(
        local,
        mesh=mesh,
        in_specs=(
            P("sp", None),
            P("sp", "tp"),
            P("sp", "tp"),
            P("sp", "tp"),
            P("sp", "tp"),
            P("tp"),
            P("sp", "tp"),
            P(),
            P("tp", None),
            P(),
            P("sp", "tp"),
            P("sp", "tp"),
            P("tp", "sp"),
        ),
        out_specs=P("sp", None),
        check_vma=False,
    )
```

```python
import jax
import jax.numpy as jnp
from jax import lax
from jax.experimental import pallas as pl
from jax.experimental.pallas import tpu as pltpu
from jax.sharding import PartitionSpec as P

HD = 128
BLOCK = 64


eps = 1e-06
top_precision = lax.Precision.HIGHEST


def carried_in_2(value, axis, join, neutral):
    place = lax.axis_index(axis)
    gathered = jax.tree.map(
        lambda a, kind: lax.all_gather(a.astype(kind), axis), value, (jnp.bfloat16, jnp.bfloat16)
    )
    state = jax.tree.map(lambda a, e: jnp.zeros_like(a) + jnp.asarray(e, a.dtype), value, neutral)

    def one(turn, state):
        return join(
            state,
            jax.tree.map(
                lambda a, own: lax.dynamic_index_in_dim(a, turn, 0, False).astype(own.dtype),
                gathered,
                value,
            ),
        )

    return lax.fori_loop(0, place, one, state)


def block_update(carried_in, inputs):
    recurrent_state, offset = carried_in
    queries, state_increment, value_rows, retain_log_factor = inputs
    running_state = jnp.cumsum(retain_log_factor, axis=1)
    causal = jnp.tril(
        jnp.ones((retain_log_factor.shape[1], retain_log_factor.shape[1]), dtype=bool)
    )
    carried_over_state = jnp.einsum(
        "uqw,uwa->uqa", queries * jnp.exp(running_state), recurrent_state, precision=top_precision
    )
    spread = running_state[:, :, None, :] - running_state[:, None, :, :]
    weights = jnp.exp(jnp.where(causal[None, :, :, None], spread, -jnp.inf))
    scores = jnp.einsum(
        "htk,htsk,hsk->hts", queries, weights, state_increment, precision=top_precision
    )
    output_rows = carried_over_state + jnp.einsum(
        "hts,hsv->htv", scores, value_rows, precision=top_precision
    )
    final_state = running_state[:, -1:, :]
    updated_state = jnp.exp(final_state[:, 0, :])[:, :, None] * recurrent_state + jnp.einsum(
        "erb,erc->ebc",
        state_increment * jnp.exp(final_state - running_state),
        value_rows,
        precision=top_precision,
    )
    rescaled_state = queries * jnp.exp(running_state + offset[:, None, :])
    return ((updated_state, offset + final_state[:, 0, :]), (output_rows, rescaled_state))


def join_states(earlier, later):
    earlier_sum, earlier_memory = earlier
    later_sum, later_memory = later
    return (earlier_sum + later_sum, jnp.exp(later_sum)[:, :, None] * earlier_memory + later_memory)


MESH = pl.DeviceIdType.MESH
GROUPS = 4


def up_to(value, step):
    return -(-value // step) * step


def layer_kernel(
    dims, gu_ref, dn_ref, q_ref, f_ref, v_ref, og_ref, margin_ref, extra_ref, head_gain_ref, ow_ref,
    residual_ref, ff_gain_ref, out_ref,
    gu, dn, grown, q_grown, plane, columns, gated, proj, proj_got, x_own, rows_in, hid, part, peer_part, summed, got,
    s_a, r_a, s_b, r_b, s_x, r_x, s_p, r_p, s_d, r_d, s_r, r_r, s_o, r_o, s_l,
    s_1, r_1, s_2, r_2, s_j, r_j,
):
    n_r, share, own, width, padded = dims
    me = lax.axis_index("sp")
    c = lax.axis_index("tp")
    h, r = me // n_r, me % n_r
    model = gu.shape[0]

    def away(d):
        return (h + d) % GROUPS

    def back(d):
        return (h + GROUPS - d) % GROUPS

    def beside(e):
        return ((r // 2 + e // 2) % 2) * 2 + (r % 2 + e % 2) % 2

    def remote(src, dst, send, recv, hh, rr, cc):
        return pltpu.make_async_remote_copy(
            src_ref=src, dst_ref=dst, send_sem=send, recv_sem=recv,
            device_id=(hh * n_r + rr, cc), device_id_type=MESH,
        )

    def gu_rows(owner):
        return gu.at[pl.ds(pl.multiple_of(owner * share, share), share)]

    def dn_cols(owner):
        return dn.at[pl.ds(0, width), pl.ds(pl.multiple_of(owner * share, share), share)]

    def token_rows(hh, cc):
        return pl.ds(pl.multiple_of((hh * 2 + cc) * own, own), own)

    started = []

    def go(copy):
        copy.start()
        started.append(copy)
        return copy

    weights_a = {}
    weights_b = {}
    mine = pl.ds(pl.multiple_of(c * own, own), own)
    theirs = pl.ds(pl.multiple_of((1 - c) * own, own), own)

    def share_out(k):
        source = (gu_ref, dn_ref)[k]
        place = (gu_rows, dn_cols)[k]
        for d in (1, 3, 2):
            weights_a[d, k] = go(remote(source.at[away(d)], place(me), s_a.at[d - 1, k], r_a.at[d - 1, k], away(d), r, c))
        for e in (1, 2, 3):
            weights_b[0, e, k] = go(remote(source.at[h], place(me), s_b.at[0, e - 1, k], r_b.at[0, e - 1, k], h, beside(e), c))

    def hand_on(d, k):
        weights_a[d, k].wait_recv()
        block = (gu_rows, dn_cols)[k](back(d) * n_r + r)
        for e in (1, 2, 3):
            weights_b[d, e, k] = go(remote(block, block, s_b.at[d, e - 1, k], r_b.at[d, e - 1, k], h, beside(e), c))

    share_out(0)
    own_gu = pltpu.make_async_copy(gu_ref.at[h], gu_rows(me), s_l.at[0])
    own_dn = pltpu.make_async_copy(dn_ref.at[h], dn_cols(me), s_l.at[1])
    own_gu.start()
    own_dn.start()
    dn[pl.ds(width, padded - width), :] = jnp.zeros((padded - width, model), dn.dtype)

    bf, f32 = jnp.bfloat16, jnp.float32
    length, channels = q_ref.shape
    heads = channels // HD
    span = 128
    ones = lambda n: lax.broadcasted_iota(jnp.int32, (n, n), 0) >= lax.broadcasted_iota(jnp.int32, (n, n), 1)
    lower = ones(length).astype(f32)
    causal = ones(span)
    over = lambda x, y, i, j: lax.dot_general(x, y, (((i,), (j,)), ((), ())), preferred_element_type=f32)
    for n in range(heads):
        cols = slice(n * HD, (n + 1) * HD)
        inflow = margin_ref[:, cols] * jax.nn.sigmoid(-f_ref[:, cols].astype(f32))
        keep = jnp.log1p(-inflow) + extra_ref[:, cols]
        total_log = lax.dot_general(lower, keep, (((1,), (0,)), ((), ())), precision=top_precision, preferred_element_type=f32)
        q = q_ref[:, cols].astype(f32)
        q_grown[:, cols] = (q * jnp.exp(total_log)).astype(bf)
        state = None
        for start in range(0, length, span):
            rows = slice(start, start + span)
            a, qb, ub, vb = total_log[rows], q[rows], inflow[rows], v_ref[rows, cols]
            middle, end = a[span // 2 - 1:span // 2], a[span - 1:span]
            scores = over((qb * jnp.exp(a - middle)).astype(bf), (ub * jnp.exp(middle - a)).astype(bf), 1, 1)
            mixed = over(jnp.where(causal, scores, 0.0).astype(bf), vb, 1, 0)
            added = over(vb, (ub * jnp.exp(end - a)).astype(bf), 0, 0)
            if state is None:
                state = added
            else:
                mixed = mixed + over((qb * jnp.exp(a - base)).astype(bf), state.astype(bf), 1, 1)
                state = state * jnp.exp(end - base) + added
            grown[rows, cols] = mixed
            base = end
        plane[r, n * HD:(n + 1) * HD, :] = state.astype(bf)
        high = base.astype(bf)
        plane[r, heads * HD + n:heads * HD + n + 1, :] = high
        plane[r, heads * HD + 8 + n:heads * HD + 9 + n, :] = (base - high.astype(f32)).astype(bf)

    across = {e: go(remote(plane.at[r], plane.at[r], s_1.at[e - 1], r_1.at[e - 1], h, beside(e), c)) for e in (1, 2, 3)}
    hand_on(1, 0)
    for e in (1, 2, 3):
        across[e].wait_recv()

    def part_of(ref, at, n):
        logs = ref[at, heads * HD + n:heads * HD + n + 1, :].astype(f32) + ref[at, heads * HD + 8 + n:heads * HD + 9 + n, :].astype(f32)
        return logs, ref[at, n * HD:(n + 1) * HD, :].astype(f32)

    before = []
    for n in range(heads):
        whole = jnp.zeros((HD, HD), f32)
        whole_log = jnp.zeros((1, HD), f32)
        early, early_log = whole, whole_log
        for at in range(n_r):
            logs, state = part_of(plane, at, n)
            whole = whole * jnp.exp(logs) + state
            whole_log = whole_log + logs
            early = jnp.where(at < r, whole, early)
            early_log = jnp.where(at < r, whole_log, early_log)
        before.append((early_log, early))
        columns[h, n * HD:(n + 1) * HD, :] = whole.astype(bf)
        high = whole_log.astype(bf)
        columns[h, heads * HD + n:heads * HD + n + 1, :] = high
        columns[h, heads * HD + 8 + n:heads * HD + 9 + n, :] = (whole_log - high.astype(f32)).astype(bf)
    along = {d: go(remote(columns.at[h], columns.at[h], s_2.at[d - 1], r_2.at[d - 1], away(d), r, c)) for d in (1, 3, 2)}
    hand_on(3, 0)
    hand_on(2, 0)
    share_out(1)
    for d in (1, 3, 2):
        along[d].wait_recv()
    for n in range(heads):
        cols = slice(n * HD, (n + 1) * HD)
        state = jnp.zeros((HD, HD), f32)
        for at in range(GROUPS - 1):
            logs, later = part_of(columns, at, n)
            state = jnp.where(at < h, state * jnp.exp(logs) + later, state)
        early_log, early = before[n]
        state = state * jnp.exp(early_log) + early
        mixed = grown[:, cols] + over(q_grown[:, cols], state.astype(bf), 1, 1)
        scale = lax.rsqrt(jnp.mean(mixed * mixed, axis=-1, keepdims=True) + eps)
        gate = og_ref[:, cols].astype(f32)
        gated[:, cols] = (mixed * scale * head_gain_ref[...] * (gate * jax.nn.sigmoid(gate))).astype(bf)

    def project(j, carry):
        at = pl.multiple_of(j * 256, 256)
        proj[:, pl.ds(at, 256)] = jnp.dot(
            gated[...], ow_ref[:, pl.ds(at, 256)], preferred_element_type=f32
        ).astype(bf)
        return carry

    lax.fori_loop(0, model // 256, project, 0)
    joined = go(remote(proj.at[theirs], proj_got, s_j.at[0], r_j.at[0], h, r, 1 - c))
    joined.wait_recv()
    x = (residual_ref[mine, :].astype(f32) + (proj[mine, :].astype(f32) + proj_got[...].astype(f32))).astype(bf)
    x_own[...] = x
    wide = x.astype(f32)
    normed = wide * lax.rsqrt(jnp.mean(wide * wide, axis=-1, keepdims=True) + eps) * ff_gain_ref[...]
    rows_in[token_rows(h, c), :] = normed.astype(bf)
    block = rows_in.at[token_rows(h, c)]
    acts = {d: go(remote(block, block, s_x.at[d - 1], r_x.at[d - 1], away(d), r, c)) for d in (1, 3, 2)}
    peers = {0: go(remote(block, block, s_p.at[0], r_p.at[0], h, r, 1 - c))}
    for d in (1, 3, 2):
        hand_on(d, 1)
    for d in (1, 3, 2):
        acts[d].wait_recv()
        block = rows_in.at[token_rows(back(d), c)]
        peers[d] = go(remote(block, block, s_p.at[d], r_p.at[d], h, r, 1 - c))
    own_gu.wait()
    own_dn.wait()
    for d in range(4):
        for e in (1, 2, 3):
            weights_b[d, e, 0].wait_recv()

    def reduce_block(d, exchange):
        exchange.wait_recv()
        here = part[d, mine, :]
        total = here.astype(jnp.float32) + peer_part[d].astype(jnp.float32)
        summed[d] = total.astype(jnp.bfloat16)
        if d == 0:
            return None
        return go(remote(summed.at[d], got.at[d - 1], s_r.at[d - 1], r_r.at[d - 1], back(d), r, c))

    tile = 256
    order = (1, 3, 2, 0)
    exchanges = {}
    reduced = {}
    for place, d in enumerate(order):
        peers[d].wait_recv()
        first = pl.multiple_of(back(d) * 2 * own, 2 * own)

        def gate_up(j, carry):
            at = pl.multiple_of(j * tile, tile)
            rows = rows_in[pl.ds(first, 2 * own), :]
            gate = jnp.dot(rows, gu[:, pl.ds(at, tile)], preferred_element_type=jnp.float32)
            up = jnp.dot(rows, gu[:, pl.ds(padded + at, tile)], preferred_element_type=jnp.float32)
            hid[:, pl.ds(at, tile)] = (gate * jax.nn.sigmoid(gate) * up).astype(jnp.bfloat16)
            return carry

        lax.fori_loop(0, padded // tile, gate_up, 0)
        if place == 0:
            for dd in range(4):
                for e in (1, 2, 3):
                    weights_b[dd, e, 1].wait_recv()

        def down(j, carry):
            at = pl.multiple_of(j * tile, tile)
            part[d, :, pl.ds(at, tile)] = jnp.dot(
                hid[...], dn[:, pl.ds(at, tile)], preferred_element_type=jnp.float32
            ).astype(jnp.bfloat16)
            return carry

        lax.fori_loop(0, model // tile, down, 0)
        exchanges[d] = go(remote(
            part.at[d, theirs], peer_part.at[d],
            s_d.at[d], r_d.at[d], h, r, 1 - c,
        ))
        if place:
            reduced[order[place - 1]] = reduce_block(order[place - 1], exchanges[order[place - 1]])
    reduce_block(0, exchanges[0])
    total = summed[0].astype(jnp.float32)
    for d in (1, 3, 2):
        reduced[d].wait_recv()
        total = total + got[d - 1].astype(jnp.float32)
    out_ref[mine, :] = (x_own[...].astype(jnp.float32) + 0.5 * total).astype(jnp.bfloat16)
    finish = go(remote(out_ref.at[mine], out_ref.at[mine], s_o.at[0], r_o.at[0], h, r, 1 - c))
    finish.wait_recv()
    for copy in started:
        copy.wait_send()


def layer(
    residual, queries, forget_gate_logits, projected_values, output_gate_logits, lower_bound_margin,
    extra_forget_logs, per_head_norm_gain, output_weight, feedforward_norm_gain, gate_weight, up_weight, down_weight,
):
    n_sp = lax.axis_size("sp")
    share, half = gate_weight.shape
    width = half // GROUPS
    padded = up_to(width, 256)
    length, model = residual.shape
    own = length // 2
    channels = queries.shape[1]
    message = channels + 16
    pad = ((0, 0), (0, 0), (0, padded - width))
    split = lambda w: jnp.pad(w.reshape(share, GROUPS, width), pad)
    gu = jnp.concatenate([split(gate_weight), split(up_weight)], axis=2).transpose(1, 0, 2)
    dn = down_weight.reshape(GROUPS, width, share)
    bf, f32 = jnp.bfloat16, jnp.float32
    dma = pltpu.SemaphoreType.DMA
    n_r = n_sp // GROUPS
    dims = (n_r, share, own, width, padded)
    vm = pl.BlockSpec(memory_space=pltpu.VMEM)
    hbm = pl.BlockSpec(memory_space=pl.ANY)
    return pl.pallas_call(
        lambda *refs: layer_kernel(dims, *refs),
        out_shape=jax.ShapeDtypeStruct((length, model), bf),
        in_specs=[hbm, hbm] + [vm] * 10,
        out_specs=vm,
        scratch_shapes=[
            pltpu.VMEM((model, 2 * padded), bf),
            pltpu.VMEM((padded, model), bf),
            pltpu.VMEM((length, channels), f32),
            pltpu.VMEM((length, channels), bf),
            pltpu.VMEM((n_r, message, HD), bf),
            pltpu.VMEM((GROUPS, message, HD), bf),
            pltpu.VMEM((length, channels), bf),
            pltpu.VMEM((length, model), bf),
            pltpu.VMEM((own, model), bf),
            pltpu.VMEM((own, model), bf),
            pltpu.VMEM((GROUPS * length, model), bf),
            pltpu.VMEM((length, padded), bf),
            pltpu.VMEM((GROUPS, length, model), bf),
            pltpu.VMEM((GROUPS, own, model), bf),
            pltpu.VMEM((GROUPS, own, model), bf),
            pltpu.VMEM((GROUPS - 1, own, model), bf),
            dma((3, 2)), dma((3, 2)), dma((4, 3, 2)), dma((4, 3, 2)),
            dma((3,)), dma((3,)), dma((4,)), dma((4,)), dma((4,)), dma((4,)),
            dma((3,)), dma((3,)), dma((1,)), dma((1,)), dma((2,)),
            dma((3,)), dma((3,)), dma((3,)), dma((3,)), dma((1,)), dma((1,)),
        ],
        compiler_params=pltpu.CompilerParams(has_side_effects=True, vmem_limit_bytes=56 * 2**20),
    )(
        gu, dn, queries, forget_gate_logits, projected_values, output_gate_logits,
        lower_bound_margin.reshape(1, channels), extra_forget_logs, per_head_norm_gain.reshape(1, HD),
        output_weight, residual, feedforward_norm_gain.reshape(1, model),
    )


def fits(residual, queries, gate_weight):
    length, model = residual.shape
    share, half = gate_weight.shape
    return (
        lax.axis_size("sp") == 4 * GROUPS and lax.axis_size("tp") == 2 and share % 128 == 0
        and length % 128 == 0 and length <= 512 and half % (16 * GROUPS) == 0
        and queries.shape[1] <= 8 * HD and model % 256 == 0
    )


def local(
    residual,
    queries,
    forget_gate_logits,
    projected_values,
    output_gate_logits,
    lower_bound_margin,
    extra_forget_logs,
    per_head_norm_gain,
    output_weight,
    feedforward_norm_gain,
    gate_weight,
    up_weight,
    down_weight,
):
    if fits(residual, queries, gate_weight):
        return layer(
            residual, queries, forget_gate_logits, projected_values, output_gate_logits, lower_bound_margin,
            extra_forget_logs, per_head_norm_gain, output_weight, feedforward_norm_gain, gate_weight, up_weight, down_weight,
        )
    length = queries.shape[0]
    head_count = queries.shape[1] // HD
    state_increment = lower_bound_margin * jax.nn.sigmoid(-forget_gate_logits.astype(jnp.float32))
    retain_log_factor = jnp.log1p(-state_increment) + extra_forget_logs

    def to_blocks(source):
        return source.reshape(length // BLOCK, BLOCK, head_count, HD).transpose(0, 2, 1, 3)

    initial = (
        jnp.zeros((head_count, HD, HD), jnp.float32),
        jnp.zeros((head_count, HD), jnp.float32),
    )
    block_inputs = (
        to_blocks(queries.astype(jnp.float32)),
        to_blocks(state_increment),
        to_blocks(projected_values.astype(jnp.float32)),
        to_blocks(retain_log_factor),
    )
    (recurrent_state, decay_sum), (output_rows, rescaled_state) = lax.scan(
        block_update, initial, block_inputs
    )
    identity = (jnp.zeros_like(decay_sum), jnp.zeros_like(recurrent_state))
    incoming_state = carried_in_2((decay_sum, recurrent_state), "sp", join_states, identity)[1]
    output_rows = output_rows + jnp.einsum(
        "sjey,jyx->sjex", rescaled_state, incoming_state, precision=top_precision
    )
    mixed = output_rows.transpose(0, 2, 1, 3).reshape(length, head_count, HD)
    normed_heads = (
        mixed
        * lax.rsqrt(jnp.mean(mixed * mixed, axis=-1, keepdims=True) + eps)
        * per_head_norm_gain
    )
    gating = jax.nn.silu(output_gate_logits.astype(jnp.float32)).reshape(length, head_count, HD)
    gated = (normed_heads * gating).reshape(length, head_count * HD).astype(jnp.bfloat16)
    row_count = residual.shape[0] // lax.axis_size("tp")
    own_rows = lax.dynamic_slice_in_dim(residual, lax.axis_index("tp") * row_count, row_count, 0)
    rows_here = gated
    projected = lax.psum_scatter(
        jnp.dot(rows_here, output_weight, preferred_element_type=jnp.float32).astype(jnp.bfloat16),
        "tp",
        scatter_dimension=0,
        tiled=True,
    ).astype(jnp.float32)
    after_mixer = (own_rows.astype(jnp.float32) + projected).astype(jnp.bfloat16)
    widened = after_mixer.astype(jnp.float32)
    normed = (
        widened
        * lax.rsqrt(jnp.mean(widened * widened, axis=-1, keepdims=True) + eps)
        * feedforward_norm_gain
    ).astype(jnp.bfloat16)
    gate_full, up_full = (
        lax.all_gather(gate_weight, "sp", axis=0, tiled=True),
        lax.all_gather(up_weight, "sp", axis=0, tiled=True),
    )
    down_full = lax.all_gather(down_weight, "sp", axis=1, tiled=True)
    row_piece = lax.all_gather(normed, "tp", axis=0, tiled=True)
    gate_part = jnp.dot(row_piece, gate_full, preferred_element_type=jnp.float32)
    up_part = jnp.dot(row_piece, up_full, preferred_element_type=jnp.float32)
    hidden = (jax.nn.silu(gate_part) * up_part).astype(jnp.bfloat16)
    rows_here = hidden
    ffn_sum = lax.psum_scatter(
        jnp.dot(rows_here, down_full, preferred_element_type=jnp.float32).astype(jnp.bfloat16),
        "tp",
        scatter_dimension=0,
        tiled=True,
    ).astype(jnp.float32)
    finished = (after_mixer.astype(jnp.float32) + 0.5 * ffn_sum).astype(jnp.bfloat16)
    return lax.all_gather(finished, "tp", axis=0, tiled=True)


def solution(mesh):
    return jax.shard_map(
        local,
        mesh=mesh,
        in_specs=(
            P("sp", None),
            P("sp", "tp"),
            P("sp", "tp"),
            P("sp", "tp"),
            P("sp", "tp"),
            P("tp"),
            P("sp", "tp"),
            P(),
            P("tp", None),
            P(),
            P("sp", "tp"),
            P("sp", "tp"),
            P("tp", "sp"),
        ),
        out_specs=P("sp", None),
        check_vma=False,
    )
```

```python
import jax
import jax.numpy as jnp
from jax import lax
from jax.experimental import pallas as pl
from jax.experimental.pallas import tpu as pltpu
from jax.sharding import PartitionSpec as P

HD = 128
BLOCK = 64


eps = 1e-06
top_precision = lax.Precision.HIGHEST


def carried_in_2(value, axis, join, neutral):
    place = lax.axis_index(axis)
    gathered = jax.tree.map(
        lambda a, kind: lax.all_gather(a.astype(kind), axis), value, (jnp.bfloat16, jnp.bfloat16)
    )
    state = jax.tree.map(lambda a, e: jnp.zeros_like(a) + jnp.asarray(e, a.dtype), value, neutral)

    def one(turn, state):
        return join(
            state,
            jax.tree.map(
                lambda a, own: lax.dynamic_index_in_dim(a, turn, 0, False).astype(own.dtype),
                gathered,
                value,
            ),
        )

    return lax.fori_loop(0, place, one, state)


def block_update(carried_in, inputs):
    recurrent_state, offset = carried_in
    queries, state_increment, value_rows, retain_log_factor = inputs
    running_state = jnp.cumsum(retain_log_factor, axis=1)
    causal = jnp.tril(
        jnp.ones((retain_log_factor.shape[1], retain_log_factor.shape[1]), dtype=bool)
    )
    carried_over_state = jnp.einsum(
        "uqw,uwa->uqa", queries * jnp.exp(running_state), recurrent_state, precision=top_precision
    )
    spread = running_state[:, :, None, :] - running_state[:, None, :, :]
    weights = jnp.exp(jnp.where(causal[None, :, :, None], spread, -jnp.inf))
    scores = jnp.einsum(
        "htk,htsk,hsk->hts", queries, weights, state_increment, precision=top_precision
    )
    output_rows = carried_over_state + jnp.einsum(
        "hts,hsv->htv", scores, value_rows, precision=top_precision
    )
    final_state = running_state[:, -1:, :]
    updated_state = jnp.exp(final_state[:, 0, :])[:, :, None] * recurrent_state + jnp.einsum(
        "erb,erc->ebc",
        state_increment * jnp.exp(final_state - running_state),
        value_rows,
        precision=top_precision,
    )
    rescaled_state = queries * jnp.exp(running_state + offset[:, None, :])
    return ((updated_state, offset + final_state[:, 0, :]), (output_rows, rescaled_state))


def join_states(earlier, later):
    earlier_sum, earlier_memory = earlier
    later_sum, later_memory = later
    return (earlier_sum + later_sum, jnp.exp(later_sum)[:, :, None] * earlier_memory + later_memory)


MESH = pl.DeviceIdType.MESH
GROUPS = 4


def up_to(value, step):
    return -(-value // step) * step


def layer_kernel(
    dims, gu_ref, dn_ref, q_ref, f_ref, v_ref, og_ref, margin_ref, extra_ref, head_gain_ref, ow_ref,
    residual_ref, ff_gain_ref, out_ref,
    gu, dn, grown, q_grown, plane, columns, gated, proj, proj_got, x_own, rows_in, hid, part, peer_part, summed, got,
    s_a, r_a, s_b, r_b, s_x, r_x, s_p, r_p, s_d, r_d, s_r, r_r, s_o, r_o, s_l,
    s_1, r_1, s_2, r_2, s_j, r_j,
):
    n_r, share, own, width, padded = dims
    me = lax.axis_index("sp")
    c = lax.axis_index("tp")
    h, r = me // n_r, me % n_r
    model = gu.shape[0]

    def away(d):
        return (h + d) % GROUPS

    def back(d):
        return (h + GROUPS - d) % GROUPS

    def beside(e):
        return ((r // 2 + e // 2) % 2) * 2 + (r % 2 + e % 2) % 2

    def remote(src, dst, send, recv, hh, rr, cc):
        return pltpu.make_async_remote_copy(
            src_ref=src, dst_ref=dst, send_sem=send, recv_sem=recv,
            device_id=(hh * n_r + rr, cc), device_id_type=MESH,
        )

    def gu_rows(owner):
        return gu.at[pl.ds(pl.multiple_of(owner * share, share), share)]

    def dn_cols(owner):
        return dn.at[pl.ds(0, width), pl.ds(pl.multiple_of(owner * share, share), share)]

    def token_rows(hh, cc):
        return pl.ds(pl.multiple_of((hh * 2 + cc) * own, own), own)

    started = []

    def go(copy):
        copy.start()
        started.append(copy)
        return copy

    weights_a = {}
    weights_b = {}
    mine = pl.ds(pl.multiple_of(c * own, own), own)
    theirs = pl.ds(pl.multiple_of((1 - c) * own, own), own)

    def share_out(k):
        source = (gu_ref, dn_ref)[k]
        place = (gu_rows, dn_cols)[k]
        for d in (1, 3, 2):
            weights_a[d, k] = go(remote(source.at[away(d)], place(me), s_a.at[d - 1, k], r_a.at[d - 1, k], away(d), r, c))
        for e in (1, 2):
            weights_b[0, e, k] = go(remote(source.at[h], place(me), s_b.at[0, e - 1, k], r_b.at[0, e - 1, k], h, beside(e), c))

    def hand_on(d, k):
        weights_a[d, k].wait_recv()
        block = (gu_rows, dn_cols)[k](back(d) * n_r + r)
        for e in (1, 2):
            weights_b[d, e, k] = go(remote(block, block, s_b.at[d, e - 1, k], r_b.at[d, e - 1, k], h, beside(e), c))

    here_already = set()

    def arrive(*key):
        if key not in here_already:
            here_already.add(key)
            weights_b[key].wait_recv()

    def relay(d, k):
        first = 1 + d % 2
        arrive(d, first, k)
        block = (gu_rows, dn_cols)[k](back(d) * n_r + beside(first))
        weights_b[d, 3, k] = go(remote(block, block, s_b.at[d, 2, k], r_b.at[d, 2, k], h, beside(3 - first), c))

    share_out(0)
    own_gu = pltpu.make_async_copy(gu_ref.at[h], gu_rows(me), s_l.at[0])
    own_dn = pltpu.make_async_copy(dn_ref.at[h], dn_cols(me), s_l.at[1])
    own_gu.start()
    own_dn.start()
    if padded > width:
        dn[pl.ds(width, padded - width), :] = jnp.zeros((padded - width, model), dn.dtype)

    bf, f32 = jnp.bfloat16, jnp.float32
    length, channels = q_ref.shape
    heads = channels // HD
    span = 128
    ones = lambda n: lax.broadcasted_iota(jnp.int32, (n, n), 0) >= lax.broadcasted_iota(jnp.int32, (n, n), 1)
    lower = ones(length).astype(f32)
    causal = ones(span)
    over = lambda x, y, i, j: lax.dot_general(x, y, (((i,), (j,)), ((), ())), preferred_element_type=f32)
    for n in range(heads):
        cols = slice(n * HD, (n + 1) * HD)
        inflow = margin_ref[:, cols] * jax.nn.sigmoid(-f_ref[:, cols].astype(f32))
        keep = jnp.log1p(-inflow) + extra_ref[:, cols]
        total_log = lax.dot_general(lower, keep, (((1,), (0,)), ((), ())), precision=top_precision, preferred_element_type=f32)
        q = q_ref[:, cols].astype(f32)
        q_grown[:, cols] = (q * jnp.exp(total_log)).astype(bf)
        state = None
        for start in range(0, length, span):
            rows = slice(start, start + span)
            a, qb, ub, vb = total_log[rows], q[rows], inflow[rows], v_ref[rows, cols]
            middle, end = a[span // 2 - 1:span // 2], a[span - 1:span]
            scores = over((qb * jnp.exp(a - middle)).astype(bf), (ub * jnp.exp(middle - a)).astype(bf), 1, 1)
            mixed = over(jnp.where(causal, scores, 0.0).astype(bf), vb, 1, 0)
            added = over(vb, (ub * jnp.exp(end - a)).astype(bf), 0, 0)
            if state is None:
                state = added
            else:
                mixed = mixed + over((qb * jnp.exp(a - base)).astype(bf), state.astype(bf), 1, 1)
                state = state * jnp.exp(end - base) + added
            grown[rows, cols] = mixed
            base = end
        plane[r, n * HD:(n + 1) * HD, :] = state.astype(bf)
        high = base.astype(bf)
        plane[r, heads * HD + n:heads * HD + n + 1, :] = high
        plane[r, heads * HD + 8 + n:heads * HD + 9 + n, :] = (base - high.astype(f32)).astype(bf)

    across = {e: go(remote(plane.at[r], plane.at[r], s_1.at[e - 1], r_1.at[e - 1], h, beside(e), c)) for e in (1, 2, 3)}
    relay(0, 0)
    hand_on(1, 0)
    for e in (1, 2, 3):
        across[e].wait_recv()

    def part_of(ref, at, n):
        logs = ref[at, heads * HD + n:heads * HD + n + 1, :].astype(f32) + ref[at, heads * HD + 8 + n:heads * HD + 9 + n, :].astype(f32)
        return logs, ref[at, n * HD:(n + 1) * HD, :].astype(f32)

    before = []
    for n in range(heads):
        whole = jnp.zeros((HD, HD), f32)
        whole_log = jnp.zeros((1, HD), f32)
        early, early_log = whole, whole_log
        for at in range(n_r):
            logs, state = part_of(plane, at, n)
            whole = whole * jnp.exp(logs) + state
            whole_log = whole_log + logs
            early = jnp.where(at < r, whole, early)
            early_log = jnp.where(at < r, whole_log, early_log)
        before.append((early_log, early))
        columns[h, n * HD:(n + 1) * HD, :] = whole.astype(bf)
        high = whole_log.astype(bf)
        columns[h, heads * HD + n:heads * HD + n + 1, :] = high
        columns[h, heads * HD + 8 + n:heads * HD + 9 + n, :] = (whole_log - high.astype(f32)).astype(bf)
    along = {d: go(remote(columns.at[h], columns.at[h], s_2.at[d - 1], r_2.at[d - 1], away(d), r, c)) for d in (1, 3, 2)}
    hand_on(3, 0)
    relay(1, 0)
    hand_on(2, 0)
    share_out(1)
    for d in (1, 3, 2):
        along[d].wait_recv()
    for n in range(heads):
        cols = slice(n * HD, (n + 1) * HD)
        state = jnp.zeros((HD, HD), f32)
        for at in range(GROUPS - 1):
            logs, later = part_of(columns, at, n)
            state = jnp.where(at < h, state * jnp.exp(logs) + later, state)
        early_log, early = before[n]
        state = state * jnp.exp(early_log) + early
        mixed = grown[:, cols] + over(q_grown[:, cols], state.astype(bf), 1, 1)
        scale = lax.rsqrt(jnp.mean(mixed * mixed, axis=-1, keepdims=True) + eps)
        gate = og_ref[:, cols].astype(f32)
        gated[:, cols] = (mixed * scale * head_gain_ref[...] * (gate * jax.nn.sigmoid(gate))).astype(bf)

    def project(j, carry):
        at = pl.multiple_of(j * 256, 256)
        proj[:, pl.ds(at, 256)] = jnp.dot(
            gated[...], ow_ref[:, pl.ds(at, 256)], preferred_element_type=f32
        ).astype(bf)
        return carry

    lax.fori_loop(0, model // 256, project, 0)
    joined = go(remote(proj.at[theirs], proj_got, s_j.at[0], r_j.at[0], h, r, 1 - c))
    joined.wait_recv()
    x = (residual_ref[mine, :].astype(f32) + (proj[mine, :].astype(f32) + proj_got[...].astype(f32))).astype(bf)
    x_own[...] = x
    wide = x.astype(f32)
    normed = wide * lax.rsqrt(jnp.mean(wide * wide, axis=-1, keepdims=True) + eps) * ff_gain_ref[...]
    rows_in[token_rows(h, c), :] = normed.astype(bf)
    block = rows_in.at[token_rows(h, c)]
    acts = {d: go(remote(block, block, s_x.at[d - 1], r_x.at[d - 1], away(d), r, c)) for d in (1, 3, 2)}
    peers = {0: go(remote(block, block, s_p.at[0], r_p.at[0], h, r, 1 - c))}
    relay(3, 0)
    hand_on(1, 1)
    relay(2, 0)
    hand_on(3, 1)
    relay(0, 1)
    hand_on(2, 1)
    for d in (1, 3, 2):
        relay(d, 1)
    for d in (1, 3, 2):
        acts[d].wait_recv()
        block = rows_in.at[token_rows(back(d), c)]
        peers[d] = go(remote(block, block, s_p.at[d], r_p.at[d], h, r, 1 - c))
    own_gu.wait()
    own_dn.wait()
    for d in range(4):
        for e in (1, 2, 3):
            arrive(d, e, 0)

    def reduce_block(d, exchange):
        exchange.wait_recv()
        here = part[d, mine, :]
        total = here.astype(jnp.float32) + peer_part[d].astype(jnp.float32)
        summed[d] = total.astype(jnp.bfloat16)
        if d == 0:
            return None
        return go(remote(summed.at[d], got.at[d - 1], s_r.at[d - 1], r_r.at[d - 1], back(d), r, c))

    tile = 256
    order = (1, 3, 2, 0)
    exchanges = {}
    reduced = {}
    for place, d in enumerate(order):
        peers[d].wait_recv()
        first = pl.multiple_of(back(d) * 2 * own, 2 * own)

        def gate_up(j, carry):
            at = pl.multiple_of(j * 256, 256)
            both = jnp.dot(rows_in[pl.ds(first, 2 * own), :], gu[:, pl.ds(at, 256)], preferred_element_type=jnp.float32)
            gate, up = both[:, :128], both[:, 128:]
            hid[:, pl.ds(pl.multiple_of(j * 128, 128), 128)] = (gate * jax.nn.sigmoid(gate) * up).astype(jnp.bfloat16)
            return carry

        lax.fori_loop(0, width // 128, gate_up, 0)
        if width % 128:
            both = jnp.dot(
                rows_in[pl.ds(first, 2 * own), :], gu[:, 2 * (width // 128 * 128):], preferred_element_type=jnp.float32
            )
            hid[:, width // 128 * 128:] = (both * jax.nn.sigmoid(both) * pltpu.roll(both, 64, 1)).astype(jnp.bfloat16)
        if place == 0:
            for dd in range(4):
                for e in (1, 2, 3):
                    arrive(dd, e, 1)

        def down(j, carry):
            at = pl.multiple_of(j * tile, tile)
            part[d, :, pl.ds(at, tile)] = jnp.dot(
                hid[...], dn[:, pl.ds(at, tile)], preferred_element_type=jnp.float32
            ).astype(jnp.bfloat16)
            return carry

        lax.fori_loop(0, model // tile, down, 0)
        exchanges[d] = go(remote(
            part.at[d, theirs], peer_part.at[d],
            s_d.at[d], r_d.at[d], h, r, 1 - c,
        ))
        if place:
            reduced[order[place - 1]] = reduce_block(order[place - 1], exchanges[order[place - 1]])
    reduce_block(0, exchanges[0])
    total = summed[0].astype(jnp.float32)
    for d in (1, 3, 2):
        reduced[d].wait_recv()
        total = total + got[d - 1].astype(jnp.float32)
    out_ref[mine, :] = (x_own[...].astype(jnp.float32) + 0.5 * total).astype(jnp.bfloat16)
    finish = go(remote(out_ref.at[mine], out_ref.at[mine], s_o.at[0], r_o.at[0], h, r, 1 - c))
    finish.wait_recv()
    for copy in started:
        copy.wait_send()


def interleave_kernel(width, gate_ref, up_ref, out_ref):
    even = width // 128 * 128
    for group in range(GROUPS):
        first = group * width
        gate, up = gate_ref[:, first:first + width], up_ref[:, first:first + width]
        for at in range(0, even, 128):
            out_ref[group, :, 2 * at:2 * at + 128] = gate[:, at:at + 128]
            out_ref[group, :, 2 * at + 128:2 * at + 256] = up[:, at:at + 128]
        if width > even:
            out_ref[group, :, 2 * even:] = jnp.concatenate([gate[:, even:], up[:, even:]], axis=1)


def layer(
    residual, queries, forget_gate_logits, projected_values, output_gate_logits, lower_bound_margin,
    extra_forget_logs, per_head_norm_gain, output_weight, feedforward_norm_gain, gate_weight, up_weight, down_weight,
):
    n_sp = lax.axis_size("sp")
    share, half = gate_weight.shape
    width = half // GROUPS
    padded = up_to(width, 128)
    length, model = residual.shape
    own = length // 2
    channels = queries.shape[1]
    message = channels + 16
    gu = pl.pallas_call(
        lambda *refs: interleave_kernel(width, *refs),
        out_shape=jax.ShapeDtypeStruct((GROUPS, share, 2 * width), jnp.bfloat16),
    )(gate_weight, up_weight)
    dn = down_weight.reshape(GROUPS, width, share)
    bf, f32 = jnp.bfloat16, jnp.float32
    dma = pltpu.SemaphoreType.DMA
    n_r = n_sp // GROUPS
    dims = (n_r, share, own, width, padded)
    vm = pl.BlockSpec(memory_space=pltpu.VMEM)
    hbm = pl.BlockSpec(memory_space=pl.ANY)
    return pl.pallas_call(
        lambda *refs: layer_kernel(dims, *refs),
        out_shape=jax.ShapeDtypeStruct((length, model), bf),
        in_specs=[hbm, hbm] + [vm] * 10,
        out_specs=vm,
        scratch_shapes=[
            pltpu.VMEM((model, 2 * width), bf),
            pltpu.VMEM((padded, model), bf),
            pltpu.VMEM((length, channels), f32),
            pltpu.VMEM((length, channels), bf),
            pltpu.VMEM((n_r, message, HD), bf),
            pltpu.VMEM((GROUPS, message, HD), bf),
            pltpu.VMEM((length, channels), bf),
            pltpu.VMEM((length, model), bf),
            pltpu.VMEM((own, model), bf),
            pltpu.VMEM((own, model), bf),
            pltpu.VMEM((GROUPS * length, model), bf),
            pltpu.VMEM((length, padded), bf),
            pltpu.VMEM((GROUPS, length, model), bf),
            pltpu.VMEM((GROUPS, own, model), bf),
            pltpu.VMEM((GROUPS, own, model), bf),
            pltpu.VMEM((GROUPS - 1, own, model), bf),
            dma((3, 2)), dma((3, 2)), dma((4, 3, 2)), dma((4, 3, 2)),
            dma((3,)), dma((3,)), dma((4,)), dma((4,)), dma((4,)), dma((4,)),
            dma((3,)), dma((3,)), dma((1,)), dma((1,)), dma((2,)),
            dma((3,)), dma((3,)), dma((3,)), dma((3,)), dma((1,)), dma((1,)),
        ],
        compiler_params=pltpu.CompilerParams(has_side_effects=True, vmem_limit_bytes=56 * 2**20),
    )(
        gu, dn, queries, forget_gate_logits, projected_values, output_gate_logits,
        lower_bound_margin.reshape(1, channels), extra_forget_logs, per_head_norm_gain.reshape(1, HD),
        output_weight, residual, feedforward_norm_gain.reshape(1, model),
    )


def fits(residual, queries, gate_weight):
    length, model = residual.shape
    share, half = gate_weight.shape
    return (
        lax.axis_size("sp") == 4 * GROUPS and lax.axis_size("tp") == 2 and share % 128 == 0
        and length % 128 == 0 and length <= 512 and half % (64 * GROUPS) == 0
        and queries.shape[1] <= 8 * HD and model % 256 == 0
    )


def local(
    residual,
    queries,
    forget_gate_logits,
    projected_values,
    output_gate_logits,
    lower_bound_margin,
    extra_forget_logs,
    per_head_norm_gain,
    output_weight,
    feedforward_norm_gain,
    gate_weight,
    up_weight,
    down_weight,
):
    if fits(residual, queries, gate_weight):
        return layer(
            residual, queries, forget_gate_logits, projected_values, output_gate_logits, lower_bound_margin,
            extra_forget_logs, per_head_norm_gain, output_weight, feedforward_norm_gain, gate_weight, up_weight, down_weight,
        )
    length = queries.shape[0]
    head_count = queries.shape[1] // HD
    state_increment = lower_bound_margin * jax.nn.sigmoid(-forget_gate_logits.astype(jnp.float32))
    retain_log_factor = jnp.log1p(-state_increment) + extra_forget_logs

    def to_blocks(source):
        return source.reshape(length // BLOCK, BLOCK, head_count, HD).transpose(0, 2, 1, 3)

    initial = (
        jnp.zeros((head_count, HD, HD), jnp.float32),
        jnp.zeros((head_count, HD), jnp.float32),
    )
    block_inputs = (
        to_blocks(queries.astype(jnp.float32)),
        to_blocks(state_increment),
        to_blocks(projected_values.astype(jnp.float32)),
        to_blocks(retain_log_factor),
    )
    (recurrent_state, decay_sum), (output_rows, rescaled_state) = lax.scan(
        block_update, initial, block_inputs
    )
    identity = (jnp.zeros_like(decay_sum), jnp.zeros_like(recurrent_state))
    incoming_state = carried_in_2((decay_sum, recurrent_state), "sp", join_states, identity)[1]
    output_rows = output_rows + jnp.einsum(
        "sjey,jyx->sjex", rescaled_state, incoming_state, precision=top_precision
    )
    mixed = output_rows.transpose(0, 2, 1, 3).reshape(length, head_count, HD)
    normed_heads = (
        mixed
        * lax.rsqrt(jnp.mean(mixed * mixed, axis=-1, keepdims=True) + eps)
        * per_head_norm_gain
    )
    gating = jax.nn.silu(output_gate_logits.astype(jnp.float32)).reshape(length, head_count, HD)
    gated = (normed_heads * gating).reshape(length, head_count * HD).astype(jnp.bfloat16)
    row_count = residual.shape[0] // lax.axis_size("tp")
    own_rows = lax.dynamic_slice_in_dim(residual, lax.axis_index("tp") * row_count, row_count, 0)
    rows_here = gated
    projected = lax.psum_scatter(
        jnp.dot(rows_here, output_weight, preferred_element_type=jnp.float32).astype(jnp.bfloat16),
        "tp",
        scatter_dimension=0,
        tiled=True,
    ).astype(jnp.float32)
    after_mixer = (own_rows.astype(jnp.float32) + projected).astype(jnp.bfloat16)
    widened = after_mixer.astype(jnp.float32)
    normed = (
        widened
        * lax.rsqrt(jnp.mean(widened * widened, axis=-1, keepdims=True) + eps)
        * feedforward_norm_gain
    ).astype(jnp.bfloat16)
    gate_full, up_full = (
        lax.all_gather(gate_weight, "sp", axis=0, tiled=True),
        lax.all_gather(up_weight, "sp", axis=0, tiled=True),
    )
    down_full = lax.all_gather(down_weight, "sp", axis=1, tiled=True)
    row_piece = lax.all_gather(normed, "tp", axis=0, tiled=True)
    gate_part = jnp.dot(row_piece, gate_full, preferred_element_type=jnp.float32)
    up_part = jnp.dot(row_piece, up_full, preferred_element_type=jnp.float32)
    hidden = (jax.nn.silu(gate_part) * up_part).astype(jnp.bfloat16)
    rows_here = hidden
    ffn_sum = lax.psum_scatter(
        jnp.dot(rows_here, down_full, preferred_element_type=jnp.float32).astype(jnp.bfloat16),
        "tp",
        scatter_dimension=0,
        tiled=True,
    ).astype(jnp.float32)
    finished = (after_mixer.astype(jnp.float32) + 0.5 * ffn_sum).astype(jnp.bfloat16)
    return lax.all_gather(finished, "tp", axis=0, tiled=True)


def solution(mesh):
    return jax.shard_map(
        local,
        mesh=mesh,
        in_specs=(
            P("sp", None),
            P("sp", "tp"),
            P("sp", "tp"),
            P("sp", "tp"),
            P("sp", "tp"),
            P("tp"),
            P("sp", "tp"),
            P(),
            P("tp", None),
            P(),
            P("sp", "tp"),
            P("sp", "tp"),
            P("tp", "sp"),
        ),
        out_specs=P("sp", None),
        check_vma=False,
    )
```
